32 devices in a mesh: rep: 2 (over x), fs: 8 (over z, y), tp: 2 (over core).
Axes of the slice: x: 2, y: 2, z: 4, core: 2. Of those that a mesh axis runs over, the one named last changes fastest.
Arguments:
- resid: bfloat16 [12288, 2048], P(('rep', 'fs', 'tp')), may hold values from -6 to 6
- mix_gain: float32 [2048], replicated, may hold values from 0.1 to 1.9
- query_weight: bfloat16 [2048, 1024], P('fs', 'tp'), may hold values from -0.125 to 0.125
- key_weight: bfloat16 [2048, 1024], P('fs', 'tp'), may hold values from -0.125 to 0.125
- value_weight: bfloat16 [2048, 2048], P('fs', 'tp'), may hold values from -0.125 to 0.125
- head_gain: float32 [2048], P('tp'), may hold values from 0.1 to 1.9
- out_weight: bfloat16 [2048, 2048], P('tp', 'fs'), may hold values from -0.125 to 0.125
- mlp_gain: float32 [2048], replicated, may hold values from 0.1 to 1.9
- gate_weight: bfloat16 [2048, 2816], P('fs', 'tp'), may hold values from -0.125 to 0.125
- up_weight: bfloat16 [2048, 2816], P('fs', 'tp'), may hold values from -0.125 to 0.125
- down_weight: bfloat16 [2816, 2048], P('tp', 'fs'), may hold values from -0.109375 to 0.109375
Outputs:
- layer_out: bfloat16 [12288, 2048], P(('rep', 'fs', 'tp'))
The draws below stay inside these ranges and needn't reach their ends.
All inputs are finite; a program needn't handle non-finite values.
Results may differ from the reference program's by a relative error of at most 0.014.
Values may be sent and summed in bfloat16 or wider, within the bound.
A program may use at most 128 MiB of HBM per device.

```python
import jax
import jax.numpy as jnp
from jax import lax

D = 2048
HEADS = 4
DK = 256
DV = 512
FF = 2816
BLOCK = 128
LEN = 768
TOKENS = 12288
N_TP = 2


def shard_levels(own_key, shape, pieces, least, top_value):
    def one(dim, parts):
        heights = jax.random.uniform(jax.random.fold_in(jax.random.fold_in(own_key, 6), dim), (parts,), jnp.float32, least / len(pieces), top_value / len(pieces))
        return jnp.repeat(jnp.exp(heights), shape[dim] // parts).reshape((-1,) + (1,) * (len(shape) - dim - 1))

    level = one(*pieces[0])
    for cut in pieces[1:]:
        level = level * one(*cut)
    return level


def noise(stream_key, dims, spread, reach, split=(), held_as=jnp.bfloat16):
    level = shard_levels(stream_key, dims, split, -0.22, 0.18) if split else 1.0
    entries = jax.random.normal(stream_key, dims, jnp.float32) * spread * level
    return jnp.minimum(jnp.maximum(entries, -reach), reach).astype(held_as)


def setup_inputs(seed: int = 0) -> dict:
    arg_keys = jax.random.split(jax.random.key(seed), 12)
    resid = noise(arg_keys[0], (TOKENS, D), 1.0, 6.0, ((0, 32),))
    mix_gain = jnp.clip(1.0 + 0.18 * jax.random.normal(arg_keys[1], (D,), jnp.float32), 0.1, 1.9)
    query_weight = noise(arg_keys[2], (D, HEADS * DK), D ** -0.5, 0.125, ((0, 8), (1, 2)))
    key_weight = noise(arg_keys[3], (D, HEADS * DK), D ** -0.5, 0.125, ((0, 8), (1, 2)))
    value_weight = noise(arg_keys[4], (D, HEADS * DV), D ** -0.5, 0.125, ((0, 8), (1, 2)))
    head_gain = jnp.clip(1.0 + 0.18 * jax.random.normal(arg_keys[5], (HEADS * DV,), jnp.float32), 0.1, 1.9)
    out_weight = noise(arg_keys[6], (HEADS * DV, D), (HEADS * DV) ** -0.5, 0.125, ((0, 2), (1, 8)))
    mlp_gain = jnp.clip(1.0 + 0.18 * jax.random.normal(arg_keys[7], (D,), jnp.float32), 0.1, 1.9)
    gate_weight = noise(arg_keys[8], (D, FF), D ** -0.5, 0.125, ((0, 8), (1, 2)))
    up_weight = noise(arg_keys[9], (D, FF), D ** -0.5, 0.125, ((0, 8), (1, 2)))
    down_weight = noise(arg_keys[10], (FF, D), FF ** -0.5, 0.109375, ((0, 2), (1, 8)))
    return {"resid": resid, "mix_gain": mix_gain, "query_weight": query_weight, "key_weight": key_weight, "value_weight": value_weight, "head_gain": head_gain, "out_weight": out_weight, "mlp_gain": mlp_gain, "gate_weight": gate_weight, "up_weight": up_weight, "down_weight": down_weight}


norm_eps = 1e-06
rope_base = 10000.0

def stored(values):
    return lax.optimization_barrier(values.astype(jnp.bfloat16)).astype(jnp.float32)

def rms_scale(values, gain):
    widened = values.astype(jnp.float32)
    scaled = widened * lax.rsqrt(lax.optimization_barrier(jnp.mean(widened * widened, axis=-1, keepdims=True)) + norm_eps)
    return (scaled * gain.astype(jnp.float32)).astype(jnp.bfloat16)

def rotate(vectors):
    length_total = vectors.shape[0]
    half_width = vectors.shape[-1] // 2
    position = jnp.arange(length_total, dtype=jnp.float32)
    inverse = 1.0 / rope_base ** jnp.linspace(0.0, 1.0, half_width, dtype=jnp.float32)
    angle = position[:, None] * inverse[None, :]
    cosine = jnp.cos(angle)[:, None, :]
    sine = jnp.sin(angle)[:, None, :]
    first = vectors[..., :half_width]
    second = vectors[..., half_width:]
    return jnp.concatenate([first * cosine - second * sine, second * cosine + first * sine], axis=-1)

def decay_tables(head_ids, block):
    log_gamma = jnp.log1p(-2.0 ** (-5.0 - 2.0 * head_ids.astype(jnp.float32)))
    offset = jnp.arange(block, dtype=jnp.float32)
    distance = offset[:, None] - offset[None, :]
    inside = jnp.where(distance >= 0, jnp.exp(log_gamma[:, None, None] * jnp.maximum(distance, 0.0)), 0.0)
    query_decay = jnp.exp(log_gamma[:, None] * (offset + 1.0))
    key_decay = jnp.exp(log_gamma[:, None] * (block - 1.0 - offset))
    block_decay = jnp.exp(log_gamma * block)
    return (inside, query_decay, key_decay, block_decay)

def retain(queries, keys, values, head_ids, block):
    length_total, heads, key_width = queries.shape
    value_width = values.shape[-1]
    count = length_total // block
    inside, query_decay, key_decay, block_decay = decay_tables(head_ids, block)

    def blocks(tensor):
        return tensor.reshape(count, block, heads, tensor.shape[-1]).transpose(0, 2, 1, 3)

    def advance(memory, inputs):
        query_tile_rows, key_tile_rows, value_block = inputs
        query_widened = query_tile_rows.astype(jnp.float32)
        value_wide = value_block.astype(jnp.float32)
        attention_scores = jnp.einsum('zvf,zjf->zvj', query_widened, key_tile_rows.astype(jnp.float32))
        weights = stored(attention_scores * inside)
        within = jnp.einsum('hlm,hmv->hlv', weights, value_wide)
        carried = jnp.einsum('hld,hdv->hlv', query_widened, stored(memory)) * query_decay[:, :, None]
        weighted_keys = stored(key_tile_rows.astype(jnp.float32) * key_decay[:, :, None])
        memory = memory * block_decay[:, None, None] + jnp.einsum('hld,hlv->hdv', weighted_keys, value_wide)
        return (memory, within + carried)
    start_state = jnp.zeros((heads, key_width, value_width), jnp.float32)
    _, outputs = lax.scan(advance, start_state, (blocks(queries), blocks(keys), blocks(values)))
    return outputs.transpose(0, 2, 1, 3).reshape(length_total, heads, value_width)

def head_scale(retained, gain):
    scaled = retained * lax.rsqrt(lax.optimization_barrier(jnp.mean(retained * retained, axis=-1, keepdims=True)) + norm_eps)
    return (scaled.reshape(retained.shape[0], -1) * gain.astype(jnp.float32)).astype(jnp.bfloat16)

def reference(resid, mix_gain, query_weight, key_weight, value_weight, head_gain, out_weight, mlp_gain, gate_weight, up_weight, down_weight):
    head_ids = jnp.arange(HEADS, dtype=jnp.int32)
    head_share = HEADS * DV // N_TP
    unit_share = FF // N_TP

    def single_sequence(token_rows):
        normed = rms_scale(token_rows, mix_gain)
        queries = stored(jnp.dot(normed, query_weight, preferred_element_type=jnp.float32)).reshape(LEN, HEADS, DK)
        keys = stored(jnp.dot(normed, key_weight, preferred_element_type=jnp.float32)).reshape(LEN, HEADS, DK)
        values = jnp.dot(normed, value_weight, preferred_element_type=jnp.float32).astype(jnp.bfloat16)
        values = values.reshape(LEN, HEADS, DV)
        query_rot = rotate(queries).astype(jnp.bfloat16)
        key_rot = (rotate(keys) * DK ** (-0.5)).astype(jnp.bfloat16)
        retained = retain(query_rot, key_rot, values, head_ids, BLOCK)
        head_out = head_scale(retained, head_gain)
        mixer_sum = jnp.zeros((LEN, D), jnp.float32)
        for group in range(N_TP):
            lower = group * head_share
            partial_sum = jnp.dot(head_out[:, lower:lower + head_share], out_weight[lower:lower + head_share], preferred_element_type=jnp.float32)
            mixer_sum = mixer_sum + stored(partial_sum)
        middle = (token_rows.astype(jnp.float32) + mixer_sum).astype(jnp.bfloat16)
        normed_mlp = rms_scale(middle, mlp_gain)
        gate = jnp.dot(normed_mlp, gate_weight, preferred_element_type=jnp.float32)
        upward = jnp.dot(normed_mlp, up_weight, preferred_element_type=jnp.float32)
        hidden_units = (jax.nn.silu(gate) * upward).astype(jnp.bfloat16)
        mlp_sum = jnp.zeros((LEN, D), jnp.float32)
        for group in range(N_TP):
            lower = group * unit_share
            partial_sum = jnp.dot(hidden_units[:, lower:lower + unit_share], down_weight[lower:lower + unit_share], preferred_element_type=jnp.float32)
            mlp_sum = mlp_sum + stored(partial_sum)
        return (middle.astype(jnp.float32) + mlp_sum).astype(jnp.bfloat16)
    sequences = resid.reshape(TOKENS // LEN, LEN, D)
    return lax.map(single_sequence, sequences).reshape(TOKENS, D)
```

```python
import functools

import jax
import jax.numpy as jnp
from jax import lax
from jax.experimental import pallas as pl
from jax.experimental.pallas import tpu as pltpu
from jax.sharding import PartitionSpec as P

UNITS = 8
MESH = pl.DeviceIdType.MESH


class Exchange:
    def __init__(self, depth, shards, fulls, axes, send_sem, recv_sem):
        self.depth = depth
        self.shards, self.fulls, self.axes = shards, fulls, axes
        self.send_sem, self.recv_sem = send_sem, recv_sem
        self.x = lax.axis_index("rep")
        fs = lax.axis_index("fs")
        self.z = fs // 2
        self.y = lax.rem(fs, 2)

    def barrier(self):
        sem = pltpu.get_barrier_semaphore()
        z, y, x = self.z, self.y, self.x
        pl.semaphore_signal(sem, inc=1, device_id={"rep": 1 - x}, device_id_type=MESH)
        pl.semaphore_signal(sem, inc=1, device_id={"fs": z * 2 + 1 - y}, device_id_type=MESH)

        @pl.when(z > 0)
        def _():
            pl.semaphore_signal(sem, inc=1, device_id={"fs": (z - 1) * 2 + y}, device_id_type=MESH)

        @pl.when(z < self.depth - 1)
        def _():
            pl.semaphore_signal(sem, inc=1, device_id={"fs": (z + 1) * 2 + y}, device_id_type=MESH)

        low = jnp.minimum(z, 1)
        high = jnp.minimum(self.depth - 1 - z, 1)
        pl.semaphore_wait(sem, 2 + low + high)

    def slot(self, w, block, start, count):
        rows, cols = self.shards[w].shape
        if self.axes[w] == 0:
            first = pl.multiple_of(block * rows + start, 16)
            return self.fulls[w].at[pl.ds(first, count), :]
        return self.fulls[w].at[
            pl.ds(pl.multiple_of(start, 16), count), pl.ds(pl.multiple_of(block * cols, 128), cols)
        ]

    def copy(self, w, kind, origin, own=False, incoming=False):
        x, y, z = self.x, self.y, self.z
        unit = self.shards[w].shape[0] // UNITS
        xs = 1 - x if incoming and kind in ("x1", "x2") else x
        start, count = {
            "up": (2 * x, 6), "down": (2 * x, 6), "y": (3 * x, 5), "x1": (6 * xs, 2), "x2": (5 * xs, 3),
        }[kind]
        start, count = start * unit, count * unit
        far = kind == "x2" or (incoming and kind == "y")
        block = origin * 2 + (1 - y if far else y)
        target = {
            "up": {"fs": (z + 1) * 2 + y},
            "down": {"fs": (z - 1) * 2 + y},
            "y": {"fs": z * 2 + 1 - y},
            "x1": {"rep": 1 - x},
            "x2": {"rep": 1 - x},
        }[kind]
        place = self.slot(w, block, start, count)
        source = place
        if own:
            source = self.shards[w].at[pl.ds(pl.multiple_of(start, 16), count), :]
        sends = ("up", "down", "y", "x1", "x2").index(kind)
        receives = (0, 0, 1, 2, 3)[sends]
        return pltpu.make_async_remote_copy(
            src_ref=source,
            dst_ref=place,
            send_sem=self.send_sem.at[w, sends, origin],
            recv_sem=self.recv_sem.at[w, receives, origin],
            device_id=target,
            device_id_type=MESH,
        )

    def each(self, t, body):
        if t == 0:
            body("own", self.z)
            return

        @pl.when(self.z - t >= 0)
        def _():
            body("up", self.z - t)

        @pl.when(self.z + t < self.depth)
        def _():
            body("down", self.z + t)

    def onward(self, w, way, origin, act):
        if way in ("own", "up"):

            @pl.when(self.z < self.depth - 1)
            def _():
                act(self.copy(w, "up", origin, own=way == "own"))

        if way in ("own", "down"):

            @pl.when(self.z > 0)
            def _():
                act(self.copy(w, "down", origin, own=way == "own"))

    def step(self, w, t):
        if t < self.depth:

            def arrive(way, origin):
                if way != "own":
                    self.copy(w, way, origin, incoming=True).wait_recv()
                self.onward(w, way, origin, lambda c: c.start())
                self.copy(w, "y", origin, own=way == "own").start()
                if way != "own":
                    self.copy(w, "x1", origin).start()

            self.each(t, arrive)
        if 1 <= t <= self.depth:

            def cross(way, origin):
                self.copy(w, "y", origin, incoming=True).wait_recv()
                self.copy(w, "x2", origin).start()

            self.each(t - 1, cross)
        if t == self.depth + 1:
            for s in range(self.depth):

                def last(way, origin):
                    if way != "own":
                        self.copy(w, "x1", origin, incoming=True).wait_recv()
                    self.copy(w, "x2", origin, incoming=True).wait_recv()

                self.each(s, last)

    def drain(self, w):
        for s in range(self.depth):

            def sent(way, origin):
                self.onward(w, way, origin, lambda c: c.wait_send())
                self.copy(w, "y", origin, own=way == "own").wait_send()
                if way != "own":
                    self.copy(w, "x1", origin).wait_send()
                self.copy(w, "x2", origin).wait_send()

            self.each(s, sent)


def gather_kernel(depth, axes, *refs):
    count = len(axes)
    shards, fulls = refs[:count], refs[count : 2 * count]
    held = refs[2 * count : 3 * count]
    send_sem, recv_sem, load_sem, store_sem = refs[3 * count :]
    ex = Exchange(depth, shards, fulls, axes, send_sem, recv_sem)
    loads = [pltpu.make_async_copy(shards[w], held[w], load_sem.at[w]) for w in range(count)]
    for copy in loads:
        copy.start()
    ex.barrier()
    fs = lax.axis_index("fs")
    stores = [
        pltpu.make_async_copy(
            held[w], ex.slot(w, fs, 0, shards[w].shape[0]), store_sem.at[w]
        )
        for w in range(count)
    ]
    pace = depth - 1
    for tick in range(pace * (count - 1) + depth + 2):
        for w in range(count):
            t = tick - pace * w
            if 0 <= t <= depth + 1:
                ex.step(w, t)
        if tick == 0:
            for load, store in zip(loads, stores):
                load.wait()
                store.start()
    for copy in stores:
        copy.wait()
    for w in range(count):
        ex.drain(w)


def gather_all(shards, axes):
    size = lax.axis_size("fs")
    fits = all(s.shape[0] % (UNITS * 16) == 0 and s.shape[1] % 128 == 0 for s in shards)
    if lax.axis_size("rep") != 2 or size % 2 or not fits:
        return [lax.all_gather(s, "fs", axis=a, tiled=True) for s, a in zip(shards, axes)]
    depth = size // 2
    count = len(shards)
    shapes = []
    for s, a in zip(shards, axes):
        shape = list(s.shape)
        shape[a] *= size
        shapes.append(jax.ShapeDtypeStruct(tuple(shape), s.dtype))
    return pl.pallas_call(
        functools.partial(gather_kernel, depth, tuple(axes)),
        out_shape=shapes,
        in_specs=[pl.BlockSpec(memory_space=pl.ANY)] * count,
        out_specs=[pl.BlockSpec(memory_space=pl.ANY)] * count,
        scratch_shapes=[pltpu.VMEM(s.shape, s.dtype) for s in shards]
        + [
            pltpu.SemaphoreType.DMA((count, 5, depth)),
            pltpu.SemaphoreType.DMA((count, 4, depth)),
            pltpu.SemaphoreType.DMA((count,)),
            pltpu.SemaphoreType.DMA((count,)),
        ],
        compiler_params=pltpu.CompilerParams(collective_id=0, has_side_effects=True),
    )(*shards)


DK = 256
DV = 512
BLOCK = 128


norm_eps = 1e-06
rope_base = 10000.0


def rms_scale(values, gain):
    widened = values.astype(jnp.float32)
    scaled = widened * lax.rsqrt(jnp.mean(widened * widened, axis=-1, keepdims=True) + norm_eps)
    return (scaled * gain).astype(jnp.bfloat16)


def rotate(vectors):
    length_total = vectors.shape[0]
    half_width = vectors.shape[-1] // 2
    position = jnp.arange(length_total, dtype=jnp.float32)
    inverse = 1.0 / rope_base ** jnp.linspace(0.0, 1.0, half_width, dtype=jnp.float32)
    angle = position[:, None] * inverse[None, :]
    cosine = jnp.cos(angle)[:, None, :]
    sine = jnp.sin(angle)[:, None, :]
    first = vectors[..., :half_width]
    second = vectors[..., half_width:]
    return jnp.concatenate(
        [first * cosine - second * sine, second * cosine + first * sine], axis=-1
    )


def decay_tables(head_ids, block):
    log_gamma = jnp.log1p(-(2.0 ** (-5.0 - 2.0 * head_ids.astype(jnp.float32))))
    offset = jnp.arange(block, dtype=jnp.float32)
    distance = offset[:, None] - offset[None, :]
    inside = jnp.where(
        distance >= 0, jnp.exp(log_gamma[:, None, None] * jnp.maximum(distance, 0.0)), 0.0
    )
    query_decay = jnp.exp(log_gamma[:, None] * (offset + 1.0))
    key_decay = jnp.exp(log_gamma[:, None] * (block - 1.0 - offset))
    block_decay = jnp.exp(log_gamma * block)
    return (inside, query_decay, key_decay, block_decay)


def retain(queries, keys, values, head_ids, block):
    length_total, heads, key_width = queries.shape
    value_width = values.shape[-1]
    count = length_total // block
    inside, query_decay, key_decay, block_decay = decay_tables(head_ids, block)

    def blocks(tensor):
        return tensor.reshape(count, block, heads, tensor.shape[-1]).transpose(0, 2, 1, 3)

    def advance(memory, inputs):
        query_tile_rows, key_tile_rows, value_block = inputs
        attention_scores = jnp.einsum(
            "zvf,zjf->zvj", query_tile_rows, key_tile_rows, preferred_element_type=jnp.float32
        )
        weights = (attention_scores * inside).astype(jnp.bfloat16)
        within = jnp.einsum(
            "hlm,hmv->hlv", weights, value_block, preferred_element_type=jnp.float32
        )
        carried = (
            jnp.einsum(
                "hld,hdv->hlv",
                query_tile_rows,
                memory.astype(jnp.bfloat16),
                preferred_element_type=jnp.float32,
            )
            * query_decay[:, :, None]
        )
        weighted_keys = (key_tile_rows.astype(jnp.float32) * key_decay[:, :, None]).astype(
            jnp.bfloat16
        )
        memory = memory * block_decay[:, None, None] + jnp.einsum(
            "hld,hlv->hdv", weighted_keys, value_block, preferred_element_type=jnp.float32
        )
        return (memory, within + carried)

    start_state = jnp.zeros((heads, key_width, value_width), jnp.float32)
    _, outputs = lax.scan(advance, start_state, (blocks(queries), blocks(keys), blocks(values)))
    return outputs.transpose(0, 2, 1, 3).reshape(length_total, heads, value_width)


def head_scale(retained, gain):
    scaled = retained * lax.rsqrt(jnp.mean(retained * retained, axis=-1, keepdims=True) + norm_eps)
    return (scaled.reshape(retained.shape[0], -1) * gain).astype(jnp.bfloat16)


def shards(
    resid,
    mix_gain,
    query_weight,
    key_weight,
    value_weight,
    head_gain,
    out_weight,
    mlp_gain,
    gate_weight,
    up_weight,
    down_weight,
):
    token_rows = resid.shape[0]
    length_total = token_rows * lax.axis_size("tp")
    key_cols = query_weight.shape[1]
    heads_here = key_cols // DK
    normed = rms_scale(resid, mix_gain)
    mixer_shard = jnp.concatenate([query_weight, key_weight, value_weight], axis=1)
    mlp_shard = jnp.concatenate([gate_weight, up_weight], axis=1)
    mixer_full, out_full, mlp_full, down_full = gather_all(
        [mixer_shard, out_weight, mlp_shard, down_weight], [0, 1, 0, 1]
    )
    projected = jnp.dot(
        lax.all_gather(normed, "tp", axis=0, tiled=True),
        mixer_full,
        preferred_element_type=jnp.float32,
    ).astype(jnp.bfloat16)
    queries = projected[:, :key_cols].astype(jnp.float32).reshape(length_total, heads_here, DK)
    keys = (
        projected[:, key_cols : 2 * key_cols]
        .astype(jnp.float32)
        .reshape(length_total, heads_here, DK)
    )
    values = projected[:, 2 * key_cols :].reshape(length_total, heads_here, DV)
    query_rot = rotate(queries).astype(jnp.bfloat16)
    key_rot = (rotate(keys) * DK ** (-0.5)).astype(jnp.bfloat16)
    head_ids = lax.axis_index("tp") * heads_here + jnp.arange(heads_here, dtype=jnp.int32)
    retained = retain(query_rot, key_rot, values, head_ids, BLOCK)
    head_out = head_scale(retained, head_gain)
    selected = head_out
    mixer_sum = lax.psum_scatter(
        jnp.dot(selected, out_full, preferred_element_type=jnp.float32).astype(jnp.bfloat16),
        "tp",
        scatter_dimension=0,
        tiled=True,
    ).astype(jnp.float32)
    middle = (resid.astype(jnp.float32) + mixer_sum).astype(jnp.bfloat16)
    normed_mlp = rms_scale(middle, mlp_gain)
    local_units = gate_weight.shape[1]
    both = jnp.dot(
        lax.all_gather(normed_mlp, "tp", axis=0, tiled=True),
        mlp_full,
        preferred_element_type=jnp.float32,
    )
    hidden_units = (jax.nn.silu(both[:, :local_units]) * both[:, local_units:]).astype(jnp.bfloat16)
    selected = hidden_units
    mlp_sum = lax.psum_scatter(
        jnp.dot(selected, down_full, preferred_element_type=jnp.float32).astype(jnp.bfloat16),
        "tp",
        scatter_dimension=0,
        tiled=True,
    ).astype(jnp.float32)
    return (middle.astype(jnp.float32) + mlp_sum).astype(jnp.bfloat16)


def solution(mesh):
    placed = (
        P(("rep", "fs", "tp"), None),
        P(),
        P("fs", "tp"),
        P("fs", "tp"),
        P("fs", "tp"),
        P("tp"),
        P("tp", "fs"),
        P(),
        P("fs", "tp"),
        P("fs", "tp"),
        P("tp", "fs"),
    )
    return jax.shard_map(
        shards, mesh=mesh, in_specs=placed, out_specs=P(("rep", "fs", "tp"), None), check_vma=False
    )
```

```python
import functools

import jax
import jax.numpy as jnp
from jax import lax
from jax.experimental import pallas as pl
from jax.experimental.pallas import tpu as pltpu
from jax.sharding import PartitionSpec as P

UNITS = 8
MESH = pl.DeviceIdType.MESH


class Exchange:
    def __init__(self, depth, shards, fulls, axes, send_sem, recv_sem):
        self.depth = depth
        self.shards, self.fulls, self.axes = shards, fulls, axes
        self.send_sem, self.recv_sem = send_sem, recv_sem
        self.x = lax.axis_index("rep")
        fs = lax.axis_index("fs")
        self.z = fs // 2
        self.y = lax.rem(fs, 2)

    def barrier(self):
        sem = pltpu.get_barrier_semaphore()
        z, y, x = self.z, self.y, self.x
        pl.semaphore_signal(sem, inc=1, device_id={"rep": 1 - x}, device_id_type=MESH)
        pl.semaphore_signal(sem, inc=1, device_id={"fs": z * 2 + 1 - y}, device_id_type=MESH)

        @pl.when(z > 0)
        def _():
            pl.semaphore_signal(sem, inc=1, device_id={"fs": (z - 1) * 2 + y}, device_id_type=MESH)

        @pl.when(z < self.depth - 1)
        def _():
            pl.semaphore_signal(sem, inc=1, device_id={"fs": (z + 1) * 2 + y}, device_id_type=MESH)

        low = jnp.minimum(z, 1)
        high = jnp.minimum(self.depth - 1 - z, 1)
        pl.semaphore_wait(sem, 2 + low + high)

    def slot(self, w, block, start, count):
        rows, cols = self.shards[w].shape
        if self.axes[w] == 0:
            first = pl.multiple_of(block * rows + start, 16)
            return self.fulls[w].at[pl.ds(first, count), :]
        return self.fulls[w].at[
            pl.ds(pl.multiple_of(start, 16), count), pl.ds(pl.multiple_of(block * cols, 128), cols)
        ]

    def copy(self, w, kind, origin, own=False, incoming=False):
        x, y, z = self.x, self.y, self.z
        unit = self.shards[w].shape[0] // UNITS
        xs = 1 - x if incoming and kind in ("x1", "x2") else x
        start, count = {
            "up": (2 * x, 6), "down": (2 * x, 6), "y": (3 * x, 5), "x1": (6 * xs, 2), "x2": (5 * xs, 3),
        }[kind]
        start, count = start * unit, count * unit
        far = kind == "x2" or (incoming and kind == "y")
        block = origin * 2 + (1 - y if far else y)
        target = {
            "up": {"fs": (z + 1) * 2 + y},
            "down": {"fs": (z - 1) * 2 + y},
            "y": {"fs": z * 2 + 1 - y},
            "x1": {"rep": 1 - x},
            "x2": {"rep": 1 - x},
        }[kind]
        place = self.slot(w, block, start, count)
        source = place
        if own:
            source = self.shards[w].at[pl.ds(pl.multiple_of(start, 16), count), :]
        sends = ("up", "down", "y", "x1", "x2").index(kind)
        receives = (0, 0, 1, 2, 3)[sends]
        return pltpu.make_async_remote_copy(
            src_ref=source,
            dst_ref=place,
            send_sem=self.send_sem.at[w, sends, origin],
            recv_sem=self.recv_sem.at[w, receives, origin],
            device_id=target,
            device_id_type=MESH,
        )

    def each(self, t, body):
        if t == 0:
            body("own", self.z)
            return

        @pl.when(self.z - t >= 0)
        def _():
            body("up", self.z - t)

        @pl.when(self.z + t < self.depth)
        def _():
            body("down", self.z + t)

    def onward(self, w, way, origin, act):
        if way in ("own", "up"):

            @pl.when(self.z < self.depth - 1)
            def _():
                act(self.copy(w, "up", origin, own=way == "own"))

        if way in ("own", "down"):

            @pl.when(self.z > 0)
            def _():
                act(self.copy(w, "down", origin, own=way == "own"))

    def step(self, w, t):
        if t < self.depth:

            def arrive(way, origin):
                if way != "own":
                    self.copy(w, way, origin, incoming=True).wait_recv()
                self.onward(w, way, origin, lambda c: c.start())
                self.copy(w, "y", origin, own=way == "own").start()
                if way != "own":
                    self.copy(w, "x1", origin).start()

            self.each(t, arrive)
        if 1 <= t <= self.depth:

            def cross(way, origin):
                self.copy(w, "y", origin, incoming=True).wait_recv()
                self.copy(w, "x2", origin).start()

            self.each(t - 1, cross)
        if t == self.depth + 1:
            for s in range(self.depth):

                def last(way, origin):
                    if way != "own":
                        self.copy(w, "x1", origin, incoming=True).wait_recv()
                    self.copy(w, "x2", origin, incoming=True).wait_recv()

                self.each(s, last)

    def drain(self, w):
        for s in range(self.depth):

            def sent(way, origin):
                self.onward(w, way, origin, lambda c: c.wait_send())
                self.copy(w, "y", origin, own=way == "own").wait_send()
                if way != "own":
                    self.copy(w, "x1", origin).wait_send()
                self.copy(w, "x2", origin).wait_send()

            self.each(s, sent)


def rotated(v, cosine, sine):
    half = v.shape[-1] // 2
    first, second = v[:, :half], v[:, half:]
    return jnp.concatenate(
        [first * cosine - second * sine, second * cosine + first * sine], axis=-1
    )


def column_dot(left, right, out, width=256):
    @pl.loop(0, out.shape[1] // width)
    def _(c):
        cols = pl.ds(pl.multiple_of(c * width, width), width)
        out[:, cols] = jnp.dot(
            left[...], right[:, cols], preferred_element_type=jnp.float32
        ).astype(out.dtype)


def retain_head(h, heads, tables, proj, memory, head_out):
    cos_ref, sin_ref, inside, query_decay, key_decay, block_decay, gain = tables
    block = inside.shape[-1]
    memory[...] = jnp.zeros_like(memory)
    q_cols = pl.ds(h * DK, DK)
    k_cols = pl.ds((heads + h) * DK, DK)
    v_cols = pl.ds(2 * heads * DK + h * DV, DV)

    @pl.loop(0, proj.shape[0] // block)
    def _(b):
        rows = pl.ds(pl.multiple_of(b * block, block), block)
        cosine, sine = cos_ref[rows, :], sin_ref[rows, :]
        q = rotated(proj[rows, q_cols].astype(jnp.float32), cosine, sine).astype(jnp.bfloat16)
        k = rotated(proj[rows, k_cols].astype(jnp.float32), cosine, sine) * DK ** (-0.5)
        k = k.astype(jnp.bfloat16)
        v = proj[rows, v_cols]
        scores = lax.dot_general(
            q, k, (((1,), (1,)), ((), ())), preferred_element_type=jnp.float32
        )
        weights = (scores * inside[h]).astype(jnp.bfloat16)
        state = memory[...]
        kept = jnp.dot(weights, v, preferred_element_type=jnp.float32) + query_decay[h] * jnp.dot(
            q, state.astype(jnp.bfloat16), preferred_element_type=jnp.float32
        )
        decayed = (k.astype(jnp.float32) * key_decay[h]).astype(jnp.bfloat16)
        memory[...] = state * block_decay[h] + lax.dot_general(
            decayed, v, (((0,), (0,)), ((), ())), preferred_element_type=jnp.float32
        )
        scale = lax.rsqrt(jnp.mean(kept * kept, axis=-1, keepdims=True) + norm_eps)
        head_out[rows, pl.ds(h * DV, DV)] = (
            kept * scale * gain[:, pl.ds(h * DV, DV)]
        ).astype(jnp.bfloat16)


def layer_kernel(depth, axes, *refs):
    count = len(axes)
    shards, refs = refs[:count], refs[count:]
    x_ref, tables, refs = refs[0], refs[1:8], refs[8:]
    fulls, part, refs = refs[:count], refs[count], refs[count + 1 :]
    held, refs = refs[:count], refs[count:]
    mixer, out_w, proj, memory, head_out, send_sem, recv_sem, load_sem, store_sem, fetch_sem = refs
    heads = tables[2].shape[0]
    ex = Exchange(depth, shards, fulls, axes, send_sem, recv_sem)
    loads = [pltpu.make_async_copy(shards[w], held[w], load_sem.at[w]) for w in range(count)]
    for copy in loads:
        copy.start()
    ex.barrier()
    fs = lax.axis_index("fs")
    stores = [
        pltpu.make_async_copy(held[w], ex.slot(w, fs, 0, shards[w].shape[0]), store_sem.at[w])
        for w in range(count)
    ]
    fetch_mixer = pltpu.make_async_copy(fulls[0], mixer, fetch_sem.at[0])
    fetch_out = pltpu.make_async_copy(fulls[1], out_w, fetch_sem.at[1])
    pace = depth - 1
    ready = depth + 1
    for tick in range(pace * (count - 1) + depth + 2):
        for w in range(count):
            t = tick - pace * w
            if 0 <= t <= depth + 1:
                ex.step(w, t)
        if tick == 0:
            for load, store in zip(loads, stores):
                load.wait()
                store.start()
        if tick == 1:
            for copy in stores:
                copy.wait()
        if tick == ready:
            fetch_mixer.start()
        if tick == ready + 1:
            fetch_mixer.wait()
            column_dot(x_ref, mixer, proj)
        for h in range(heads):
            if tick == ready + 2 + h // (heads // 2 if heads > 1 else 1):
                retain_head(h, heads, tables, proj, memory, head_out)
        if tick == pace + ready:
            fetch_out.start()
        if tick == pace + ready + 1:
            fetch_out.wait()
            column_dot(head_out, out_w, part)
    for w in range(count):
        ex.drain(w)


def fits(shards):
    whole = all(s.shape[0] % (UNITS * 16) == 0 and s.shape[1] % 128 == 0 for s in shards)
    return whole and lax.axis_size("rep") == 2 and lax.axis_size("fs") == 8


def layer_start(shards, axes, normed, tables):
    size = lax.axis_size("fs")
    depth = size // 2
    count = len(shards)
    shapes = []
    for s, a in zip(shards, axes):
        shape = list(s.shape)
        shape[a] *= size
        shapes.append(jax.ShapeDtypeStruct(tuple(shape), s.dtype))
    rows = normed.shape[0]
    values = shapes[1].shape[0]
    part = jax.ShapeDtypeStruct((rows, shapes[1].shape[1]), jnp.bfloat16)
    near = pl.BlockSpec(memory_space=pltpu.VMEM)
    far = pl.BlockSpec(memory_space=pl.ANY)
    return pl.pallas_call(
        functools.partial(layer_kernel, depth, tuple(axes)),
        out_shape=shapes + [part],
        in_specs=[far] * count + [near] * (1 + len(tables)),
        out_specs=[far] * count + [near],
        scratch_shapes=[pltpu.VMEM(s.shape, s.dtype) for s in shards]
        + [
            pltpu.VMEM(shapes[0].shape, jnp.bfloat16),
            pltpu.VMEM(shapes[1].shape, jnp.bfloat16),
            pltpu.VMEM((rows, shapes[0].shape[1]), jnp.bfloat16),
            pltpu.VMEM((DK, DV), jnp.float32),
            pltpu.VMEM((rows, values), jnp.bfloat16),
            pltpu.SemaphoreType.DMA((count, 5, depth)),
            pltpu.SemaphoreType.DMA((count, 4, depth)),
            pltpu.SemaphoreType.DMA((count,)),
            pltpu.SemaphoreType.DMA((count,)),
            pltpu.SemaphoreType.DMA((2,)),
        ],
        compiler_params=pltpu.CompilerParams(collective_id=0, has_side_effects=True),
    )(*shards, normed, *tables)


DK = 256
DV = 512
BLOCK = 128


norm_eps = 1e-06
rope_base = 10000.0


def rms_scale(values, gain):
    widened = values.astype(jnp.float32)
    scaled = widened * lax.rsqrt(jnp.mean(widened * widened, axis=-1, keepdims=True) + norm_eps)
    return (scaled * gain).astype(jnp.bfloat16)


def rotation(length_total, half_width):
    position = jnp.arange(length_total, dtype=jnp.float32)
    inverse = 1.0 / rope_base ** jnp.linspace(0.0, 1.0, half_width, dtype=jnp.float32)
    angle = position[:, None] * inverse[None, :]
    return (jnp.cos(angle), jnp.sin(angle))


def rotate(vectors):
    length_total = vectors.shape[0]
    half_width = vectors.shape[-1] // 2
    cosine, sine = rotation(length_total, half_width)
    cosine, sine = cosine[:, None, :], sine[:, None, :]
    first = vectors[..., :half_width]
    second = vectors[..., half_width:]
    return jnp.concatenate(
        [first * cosine - second * sine, second * cosine + first * sine], axis=-1
    )


def decay_tables(head_ids, block):
    log_gamma = jnp.log1p(-(2.0 ** (-5.0 - 2.0 * head_ids.astype(jnp.float32))))
    offset = jnp.arange(block, dtype=jnp.float32)
    distance = offset[:, None] - offset[None, :]
    inside = jnp.where(
        distance >= 0, jnp.exp(log_gamma[:, None, None] * jnp.maximum(distance, 0.0)), 0.0
    )
    query_decay = jnp.exp(log_gamma[:, None] * (offset + 1.0))
    key_decay = jnp.exp(log_gamma[:, None] * (block - 1.0 - offset))
    block_decay = jnp.exp(log_gamma * block)
    return (inside, query_decay, key_decay, block_decay)


def retain(queries, keys, values, head_ids, block):
    length_total, heads, key_width = queries.shape
    value_width = values.shape[-1]
    count = length_total // block
    inside, query_decay, key_decay, block_decay = decay_tables(head_ids, block)

    def blocks(tensor):
        return tensor.reshape(count, block, heads, tensor.shape[-1]).transpose(0, 2, 1, 3)

    def advance(memory, inputs):
        query_tile_rows, key_tile_rows, value_block = inputs
        attention_scores = jnp.einsum(
            "zvf,zjf->zvj", query_tile_rows, key_tile_rows, preferred_element_type=jnp.float32
        )
        weights = (attention_scores * inside).astype(jnp.bfloat16)
        within = jnp.einsum(
            "hlm,hmv->hlv", weights, value_block, preferred_element_type=jnp.float32
        )
        carried = (
            jnp.einsum(
                "hld,hdv->hlv",
                query_tile_rows,
                memory.astype(jnp.bfloat16),
                preferred_element_type=jnp.float32,
            )
            * query_decay[:, :, None]
        )
        weighted_keys = (key_tile_rows.astype(jnp.float32) * key_decay[:, :, None]).astype(
            jnp.bfloat16
        )
        memory = memory * block_decay[:, None, None] + jnp.einsum(
            "hld,hlv->hdv", weighted_keys, value_block, preferred_element_type=jnp.float32
        )
        return (memory, within + carried)

    start_state = jnp.zeros((heads, key_width, value_width), jnp.float32)
    _, outputs = lax.scan(advance, start_state, (blocks(queries), blocks(keys), blocks(values)))
    return outputs.transpose(0, 2, 1, 3).reshape(length_total, heads, value_width)


def head_scale(retained, gain):
    scaled = retained * lax.rsqrt(jnp.mean(retained * retained, axis=-1, keepdims=True) + norm_eps)
    return (scaled.reshape(retained.shape[0], -1) * gain).astype(jnp.bfloat16)


def shards(
    resid,
    mix_gain,
    query_weight,
    key_weight,
    value_weight,
    head_gain,
    out_weight,
    mlp_gain,
    gate_weight,
    up_weight,
    down_weight,
):
    token_rows = resid.shape[0]
    length_total = token_rows * lax.axis_size("tp")
    key_cols = query_weight.shape[1]
    heads_here = key_cols // DK
    normed = rms_scale(resid, mix_gain)
    mixer_shard = jnp.concatenate([query_weight, key_weight, value_weight], axis=1)
    mlp_shard = jnp.concatenate([gate_weight, up_weight], axis=1)
    normed_full = lax.all_gather(normed, "tp", axis=0, tiled=True)
    head_ids = lax.axis_index("tp") * heads_here + jnp.arange(heads_here, dtype=jnp.int32)
    pieces = [mixer_shard, out_weight, mlp_shard, down_weight]
    if fits(pieces) and length_total % BLOCK == 0:
        inside, query_decay, key_decay, block_decay = decay_tables(head_ids, BLOCK)
        tables = [
            *rotation(length_total, DK // 2),
            inside,
            query_decay[:, :, None],
            key_decay[:, :, None],
            jnp.broadcast_to(block_decay[:, None, None], (heads_here, DK, 1)),
            head_gain[None, :],
        ]
        _, _, mlp_full, down_full, part = layer_start(pieces, [0, 1, 0, 1], normed_full, tables)
    else:
        mixer_full, out_full, mlp_full, down_full = (
            lax.all_gather(s, "fs", axis=a, tiled=True) for s, a in zip(pieces, [0, 1, 0, 1])
        )
        projected = jnp.dot(
            normed_full, mixer_full, preferred_element_type=jnp.float32
        ).astype(jnp.bfloat16)
        both_keys = projected[:, : 2 * key_cols].astype(jnp.float32)
        both_keys = both_keys.reshape(length_total, 2, heads_here, DK)
        values = projected[:, 2 * key_cols :].reshape(length_total, heads_here, DV)
        query_rot = rotate(both_keys[:, 0]).astype(jnp.bfloat16)
        key_rot = (rotate(both_keys[:, 1]) * DK ** (-0.5)).astype(jnp.bfloat16)
        retained = retain(query_rot, key_rot, values, head_ids, BLOCK)
        head_out = head_scale(retained, head_gain)
        part = jnp.dot(head_out, out_full, preferred_element_type=jnp.float32).astype(jnp.bfloat16)
    mixer_sum = lax.psum_scatter(part, "tp", scatter_dimension=0, tiled=True).astype(jnp.float32)
    middle = (resid.astype(jnp.float32) + mixer_sum).astype(jnp.bfloat16)
    normed_mlp = rms_scale(middle, mlp_gain)
    local_units = gate_weight.shape[1]
    both = jnp.dot(
        lax.all_gather(normed_mlp, "tp", axis=0, tiled=True),
        mlp_full,
        preferred_element_type=jnp.float32,
    )
    hidden_units = (jax.nn.silu(both[:, :local_units]) * both[:, local_units:]).astype(jnp.bfloat16)
    selected = hidden_units
    mlp_sum = lax.psum_scatter(
        jnp.dot(selected, down_full, preferred_element_type=jnp.float32).astype(jnp.bfloat16),
        "tp",
        scatter_dimension=0,
        tiled=True,
    ).astype(jnp.float32)
    return (middle.astype(jnp.float32) + mlp_sum).astype(jnp.bfloat16)


def solution(mesh):
    placed = (
        P(("rep", "fs", "tp"), None),
        P(),
        P("fs", "tp"),
        P("fs", "tp"),
        P("fs", "tp"),
        P("tp"),
        P("tp", "fs"),
        P(),
        P("fs", "tp"),
        P("fs", "tp"),
        P("tp", "fs"),
    )
    return jax.shard_map(
        shards, mesh=mesh, in_specs=placed, out_specs=P(("rep", "fs", "tp"), None), check_vma=False
    )
```

```python
import functools

import jax
import jax.numpy as jnp
from jax import lax
from jax.experimental import pallas as pl
from jax.experimental.pallas import tpu as pltpu
from jax.sharding import PartitionSpec as P

UNITS = 8
MESH = pl.DeviceIdType.MESH


class Exchange:
    def __init__(self, depth, shards, fulls, axes, send_sem, recv_sem):
        self.depth = depth
        self.shards, self.fulls, self.axes = shards, fulls, axes
        self.send_sem, self.recv_sem = send_sem, recv_sem
        self.x = lax.axis_index("rep")
        fs = lax.axis_index("fs")
        self.z = fs // 2
        self.y = lax.rem(fs, 2)

    def barrier(self):
        sem = pltpu.get_barrier_semaphore()
        z, y, x = self.z, self.y, self.x
        pl.semaphore_signal(sem, inc=1, device_id={"rep": 1 - x}, device_id_type=MESH)
        pl.semaphore_signal(sem, inc=1, device_id={"fs": z * 2 + 1 - y}, device_id_type=MESH)

        @pl.when(z > 0)
        def _():
            pl.semaphore_signal(sem, inc=1, device_id={"fs": (z - 1) * 2 + y}, device_id_type=MESH)

        @pl.when(z < self.depth - 1)
        def _():
            pl.semaphore_signal(sem, inc=1, device_id={"fs": (z + 1) * 2 + y}, device_id_type=MESH)

        low = jnp.minimum(z, 1)
        high = jnp.minimum(self.depth - 1 - z, 1)
        pl.semaphore_wait(sem, 2 + low + high)

    def slot(self, w, block, start, count):
        rows, cols = self.shards[w].shape
        if self.axes[w] == 0:
            first = pl.multiple_of(block * rows + start, 16)
            return self.fulls[w].at[pl.ds(first, count), :]
        return self.fulls[w].at[
            pl.ds(pl.multiple_of(start, 16), count), pl.ds(pl.multiple_of(block * cols, 128), cols)
        ]

    def copy(self, w, kind, origin, own=False, incoming=False):
        x, y, z = self.x, self.y, self.z
        unit = self.shards[w].shape[0] // UNITS
        xs = 1 - x if incoming and kind in ("x1", "x2") else x
        start, count = {
            "up": (2 * x, 6), "down": (2 * x, 6), "y": (3 * x, 5), "x1": (6 * xs, 2), "x2": (5 * xs, 3),
        }[kind]
        start, count = start * unit, count * unit
        far = kind == "x2" or (incoming and kind == "y")
        block = origin * 2 + (1 - y if far else y)
        target = {
            "up": {"fs": (z + 1) * 2 + y},
            "down": {"fs": (z - 1) * 2 + y},
            "y": {"fs": z * 2 + 1 - y},
            "x1": {"rep": 1 - x},
            "x2": {"rep": 1 - x},
        }[kind]
        place = self.slot(w, block, start, count)
        source = place
        if own:
            source = self.shards[w].at[pl.ds(pl.multiple_of(start, 16), count), :]
        sends = ("up", "down", "y", "x1", "x2").index(kind)
        receives = (0, 0, 1, 2, 3)[sends]
        return pltpu.make_async_remote_copy(
            src_ref=source,
            dst_ref=place,
            send_sem=self.send_sem.at[w, sends, origin],
            recv_sem=self.recv_sem.at[w, receives, origin],
            device_id=target,
            device_id_type=MESH,
        )

    def each(self, t, body):
        if t == 0:
            body("own", self.z)
            return

        @pl.when(self.z - t >= 0)
        def _():
            body("up", self.z - t)

        @pl.when(self.z + t < self.depth)
        def _():
            body("down", self.z + t)

    def onward(self, w, way, origin, act):
        if way in ("own", "up"):

            @pl.when(self.z < self.depth - 1)
            def _():
                act(self.copy(w, "up", origin, own=way == "own"))

        if way in ("own", "down"):

            @pl.when(self.z > 0)
            def _():
                act(self.copy(w, "down", origin, own=way == "own"))

    def step(self, w, t):
        if t < self.depth:

            def arrive(way, origin):
                if way != "own":
                    self.copy(w, way, origin, incoming=True).wait_recv()
                self.onward(w, way, origin, lambda c: c.start())
                self.copy(w, "y", origin, own=way == "own").start()
                if way != "own":
                    self.copy(w, "x1", origin).start()

            self.each(t, arrive)
        if 1 <= t <= self.depth:

            def cross(way, origin):
                self.copy(w, "y", origin, incoming=True).wait_recv()
                self.copy(w, "x2", origin).start()

            self.each(t - 1, cross)
        if t == self.depth + 1:
            for s in range(self.depth):

                def last(way, origin):
                    if way != "own":
                        self.copy(w, "x1", origin, incoming=True).wait_recv()
                    self.copy(w, "x2", origin, incoming=True).wait_recv()

                self.each(s, last)

    def drain(self, w):
        for s in range(self.depth):

            def sent(way, origin):
                self.onward(w, way, origin, lambda c: c.wait_send())
                self.copy(w, "y", origin, own=way == "own").wait_send()
                if way != "own":
                    self.copy(w, "x1", origin).wait_send()
                self.copy(w, "x2", origin).wait_send()

            self.each(s, sent)


def rotated(v, cosine, sine):
    half = v.shape[-1] // 2
    first, second = v[:, :half], v[:, half:]
    return jnp.concatenate(
        [first * cosine - second * sine, second * cosine + first * sine], axis=-1
    )


def column_dot(left, right, out, width=256):
    @pl.loop(0, out.shape[1] // width)
    def _(c):
        cols = pl.ds(pl.multiple_of(c * width, width), width)
        out[:, cols] = jnp.dot(
            left[...], right[:, cols], preferred_element_type=jnp.float32
        ).astype(out.dtype)


def retain_head(h, heads, tables, proj, memory, head_out):
    cos_ref, sin_ref, inside, query_decay, key_decay, block_decay, gain = tables
    block = inside.shape[-1]
    memory[...] = jnp.zeros_like(memory)
    q_cols = pl.ds(h * DK, DK)
    k_cols = pl.ds((heads + h) * DK, DK)
    v_cols = pl.ds(2 * heads * DK + h * DV, DV)

    @pl.loop(0, proj.shape[0] // block)
    def _(b):
        rows = pl.ds(pl.multiple_of(b * block, block), block)
        cosine, sine = cos_ref[rows, :], sin_ref[rows, :]
        q = rotated(proj[rows, q_cols].astype(jnp.float32), cosine, sine).astype(jnp.bfloat16)
        k = rotated(proj[rows, k_cols].astype(jnp.float32), cosine, sine) * DK ** (-0.5)
        k = k.astype(jnp.bfloat16)
        v = proj[rows, v_cols]
        scores = lax.dot_general(
            q, k, (((1,), (1,)), ((), ())), preferred_element_type=jnp.float32
        )
        weights = (scores * inside[h]).astype(jnp.bfloat16)
        state = memory[...]
        kept = jnp.dot(weights, v, preferred_element_type=jnp.float32) + query_decay[h] * jnp.dot(
            q, state.astype(jnp.bfloat16), preferred_element_type=jnp.float32
        )
        decayed = (k.astype(jnp.float32) * key_decay[h]).astype(jnp.bfloat16)
        memory[...] = state * block_decay[h] + lax.dot_general(
            decayed, v, (((0,), (0,)), ((), ())), preferred_element_type=jnp.float32
        )
        scale = lax.rsqrt(jnp.mean(kept * kept, axis=-1, keepdims=True) + norm_eps)
        head_out[rows, pl.ds(h * DV, DV)] = (
            kept * scale * gain[:, pl.ds(h * DV, DV)]
        ).astype(jnp.bfloat16)


def layer_kernel(depth, axes, *refs):
    count = len(axes)
    shards, refs = refs[:count], refs[count:]
    x_ref, tables, refs = refs[0], refs[1:8], refs[8:]
    fulls, part, refs = refs[:count], refs[count], refs[count + 1 :]
    held, refs = refs[:count], refs[count:]
    mixer, out_w, proj, memory, head_out, send_sem, recv_sem, load_sem, store_sem, fetch_sem = refs
    heads = tables[2].shape[0]
    ex = Exchange(depth, shards, fulls, axes, send_sem, recv_sem)
    loads = [pltpu.make_async_copy(shards[w], held[w], load_sem.at[w]) for w in range(count)]
    for copy in loads:
        copy.start()
    ex.barrier()
    fs = lax.axis_index("fs")
    stores = [
        pltpu.make_async_copy(held[w], ex.slot(w, fs, 0, shards[w].shape[0]), store_sem.at[w])
        for w in range(count)
    ]
    fetch_mixer = pltpu.make_async_copy(fulls[0], mixer, fetch_sem.at[0])
    fetch_out = pltpu.make_async_copy(fulls[1], out_w, fetch_sem.at[1])
    pace = depth - 1
    ready = depth + 1
    for tick in range(pace * (count - 1) + depth + 2):
        for w in range(count):
            t = tick - pace * w
            if 0 <= t <= depth + 1:
                ex.step(w, t)
        if tick == 0:
            for load, store in zip(loads, stores):
                load.wait()
                store.start()
        if tick == 1:
            for copy in stores:
                copy.wait()
        if tick == ready:
            fetch_mixer.start()
        if tick == ready + 1:
            fetch_mixer.wait()
            column_dot(x_ref, mixer, proj)
        for h in range(heads):
            if tick == ready + 2 + h // (heads // 2 if heads > 1 else 1):
                retain_head(h, heads, tables, proj, memory, head_out)
        if tick == pace + ready:
            fetch_out.start()
        if tick == pace + ready + 1:
            fetch_out.wait()
            column_dot(head_out, out_w, part)
    for w in range(count):
        ex.drain(w)


def fits(shards):
    whole = all(s.shape[0] % (UNITS * 16) == 0 and s.shape[1] % 128 == 0 for s in shards)
    return whole and lax.axis_size("rep") == 2 and lax.axis_size("fs") == 8


def layer_start(shards, axes, normed, tables):
    size = lax.axis_size("fs")
    depth = size // 2
    count = len(shards)
    shapes = []
    for s, a in zip(shards, axes):
        shape = list(s.shape)
        shape[a] *= size
        shapes.append(jax.ShapeDtypeStruct(tuple(shape), s.dtype))
    rows = normed.shape[0]
    values = shapes[1].shape[0]
    part = jax.ShapeDtypeStruct((rows, shapes[1].shape[1]), jnp.bfloat16)
    near = pl.BlockSpec(memory_space=pltpu.VMEM)
    far = pl.BlockSpec(memory_space=pl.ANY)
    return pl.pallas_call(
        functools.partial(layer_kernel, depth, tuple(axes)),
        out_shape=shapes + [part],
        in_specs=[far] * count + [near] * (1 + len(tables)),
        out_specs=[far] * count + [near],
        scratch_shapes=[pltpu.VMEM(s.shape, s.dtype) for s in shards]
        + [
            pltpu.VMEM(shapes[0].shape, jnp.bfloat16),
            pltpu.VMEM(shapes[1].shape, jnp.bfloat16),
            pltpu.VMEM((rows, shapes[0].shape[1]), jnp.bfloat16),
            pltpu.VMEM((DK, DV), jnp.float32),
            pltpu.VMEM((rows, values), jnp.bfloat16),
            pltpu.SemaphoreType.DMA((count, 5, depth)),
            pltpu.SemaphoreType.DMA((count, 4, depth)),
            pltpu.SemaphoreType.DMA((count,)),
            pltpu.SemaphoreType.DMA((count,)),
            pltpu.SemaphoreType.DMA((2,)),
        ],
        compiler_params=pltpu.CompilerParams(collective_id=0, has_side_effects=True),
    )(*shards, normed, *tables)


DK = 256
DV = 512
BLOCK = 128


norm_eps = 1e-06
rope_base = 10000.0


def rms_scale(values, gain):
    widened = values.astype(jnp.float32)
    scaled = widened * lax.rsqrt(jnp.mean(widened * widened, axis=-1, keepdims=True) + norm_eps)
    return (scaled * gain).astype(jnp.bfloat16)


def rotation(length_total, half_width):
    position = jnp.arange(length_total, dtype=jnp.float32)
    inverse = 1.0 / rope_base ** jnp.linspace(0.0, 1.0, half_width, dtype=jnp.float32)
    angle = position[:, None] * inverse[None, :]
    return (jnp.cos(angle), jnp.sin(angle))


def rotate(vectors):
    length_total = vectors.shape[0]
    half_width = vectors.shape[-1] // 2
    cosine, sine = rotation(length_total, half_width)
    cosine, sine = cosine[:, None, :], sine[:, None, :]
    first = vectors[..., :half_width]
    second = vectors[..., half_width:]
    return jnp.concatenate(
        [first * cosine - second * sine, second * cosine + first * sine], axis=-1
    )


def decay_tables(head_ids, block):
    log_gamma = jnp.log1p(-(2.0 ** (-5.0 - 2.0 * head_ids.astype(jnp.float32))))
    offset = jnp.arange(block, dtype=jnp.float32)
    distance = offset[:, None] - offset[None, :]
    inside = jnp.where(
        distance >= 0, jnp.exp(log_gamma[:, None, None] * jnp.maximum(distance, 0.0)), 0.0
    )
    query_decay = jnp.exp(log_gamma[:, None] * (offset + 1.0))
    key_decay = jnp.exp(log_gamma[:, None] * (block - 1.0 - offset))
    block_decay = jnp.exp(log_gamma * block)
    return (inside, query_decay, key_decay, block_decay)


def retain(queries, keys, values, head_ids, block):
    length_total, heads, key_width = queries.shape
    value_width = values.shape[-1]
    count = length_total // block
    inside, query_decay, key_decay, block_decay = decay_tables(head_ids, block)

    def blocks(tensor):
        return tensor.reshape(count, block, heads, tensor.shape[-1]).transpose(0, 2, 1, 3)

    def advance(memory, inputs):
        query_tile_rows, key_tile_rows, value_block = inputs
        attention_scores = jnp.einsum(
            "zvf,zjf->zvj", query_tile_rows, key_tile_rows, preferred_element_type=jnp.float32
        )
        weights = (attention_scores * inside).astype(jnp.bfloat16)
        within = jnp.einsum(
            "hlm,hmv->hlv", weights, value_block, preferred_element_type=jnp.float32
        )
        carried = (
            jnp.einsum(
                "hld,hdv->hlv",
                query_tile_rows,
                memory.astype(jnp.bfloat16),
                preferred_element_type=jnp.float32,
            )
            * query_decay[:, :, None]
        )
        weighted_keys = (key_tile_rows.astype(jnp.float32) * key_decay[:, :, None]).astype(
            jnp.bfloat16
        )
        memory = memory * block_decay[:, None, None] + jnp.einsum(
            "hld,hlv->hdv", weighted_keys, value_block, preferred_element_type=jnp.float32
        )
        return (memory, within + carried)

    start_state = jnp.zeros((heads, key_width, value_width), jnp.float32)
    _, outputs = lax.scan(advance, start_state, (blocks(queries), blocks(keys), blocks(values)))
    return outputs.transpose(0, 2, 1, 3).reshape(length_total, heads, value_width)


def head_scale(retained, gain):
    scaled = retained * lax.rsqrt(jnp.mean(retained * retained, axis=-1, keepdims=True) + norm_eps)
    return (scaled.reshape(retained.shape[0], -1) * gain).astype(jnp.bfloat16)


def swap(rows):
    return lax.ppermute(rows, "tp", [(0, 1), (1, 0)])


def join_rows(rows):
    if lax.axis_size("tp") != 2:
        return lax.all_gather(rows, "tp", axis=0, tiled=True)
    first = lax.axis_index("tp") == 0
    got = swap(rows)
    return jnp.concatenate([jnp.where(first, rows, got), jnp.where(first, got, rows)], axis=0)


def share_sum(part):
    if lax.axis_size("tp") != 2:
        summed = lax.psum_scatter(part, "tp", scatter_dimension=0, tiled=True)
        return summed.astype(jnp.float32)
    count = part.shape[0] // 2
    me = lax.axis_index("tp")
    mine = lax.dynamic_slice_in_dim(part, me * count, count, axis=0)
    theirs = lax.dynamic_slice_in_dim(part, (1 - me) * count, count, axis=0)
    return mine.astype(jnp.float32) + swap(theirs).astype(jnp.float32)


def shards(
    resid,
    mix_gain,
    query_weight,
    key_weight,
    value_weight,
    head_gain,
    out_weight,
    mlp_gain,
    gate_weight,
    up_weight,
    down_weight,
):
    token_rows = resid.shape[0]
    length_total = token_rows * lax.axis_size("tp")
    key_cols = query_weight.shape[1]
    heads_here = key_cols // DK
    normed = rms_scale(resid, mix_gain)
    mixer_shard = jnp.concatenate([query_weight, key_weight, value_weight], axis=1)
    mlp_shard = jnp.concatenate([gate_weight, up_weight], axis=1)
    normed_full = join_rows(normed)
    head_ids = lax.axis_index("tp") * heads_here + jnp.arange(heads_here, dtype=jnp.int32)
    pieces = [mixer_shard, out_weight, mlp_shard, down_weight]
    if fits(pieces) and length_total % BLOCK == 0:
        inside, query_decay, key_decay, block_decay = decay_tables(head_ids, BLOCK)
        tables = [
            *rotation(length_total, DK // 2),
            inside,
            query_decay[:, :, None],
            key_decay[:, :, None],
            jnp.broadcast_to(block_decay[:, None, None], (heads_here, DK, 1)),
            head_gain[None, :],
        ]
        _, _, mlp_full, down_full, part = layer_start(pieces, [0, 1, 0, 1], normed_full, tables)
    else:
        mixer_full, out_full, mlp_full, down_full = (
            lax.all_gather(s, "fs", axis=a, tiled=True) for s, a in zip(pieces, [0, 1, 0, 1])
        )
        projected = jnp.dot(
            normed_full, mixer_full, preferred_element_type=jnp.float32
        ).astype(jnp.bfloat16)
        both_keys = projected[:, : 2 * key_cols].astype(jnp.float32)
        both_keys = both_keys.reshape(length_total, 2, heads_here, DK)
        values = projected[:, 2 * key_cols :].reshape(length_total, heads_here, DV)
        query_rot = rotate(both_keys[:, 0]).astype(jnp.bfloat16)
        key_rot = (rotate(both_keys[:, 1]) * DK ** (-0.5)).astype(jnp.bfloat16)
        retained = retain(query_rot, key_rot, values, head_ids, BLOCK)
        head_out = head_scale(retained, head_gain)
        part = jnp.dot(head_out, out_full, preferred_element_type=jnp.float32).astype(jnp.bfloat16)
    mixer_sum = share_sum(part)
    middle = (resid.astype(jnp.float32) + mixer_sum).astype(jnp.bfloat16)
    normed_mlp = rms_scale(middle, mlp_gain)
    local_units = gate_weight.shape[1]
    both = jnp.dot(
        join_rows(normed_mlp),
        mlp_full,
        preferred_element_type=jnp.float32,
    )
    hidden_units = (jax.nn.silu(both[:, :local_units]) * both[:, local_units:]).astype(jnp.bfloat16)
    selected = hidden_units
    mlp_sum = share_sum(
        jnp.dot(selected, down_full, preferred_element_type=jnp.float32).astype(jnp.bfloat16)
    )
    return (middle.astype(jnp.float32) + mlp_sum).astype(jnp.bfloat16)


def solution(mesh):
    placed = (
        P(("rep", "fs", "tp"), None),
        P(),
        P("fs", "tp"),
        P("fs", "tp"),
        P("fs", "tp"),
        P("tp"),
        P("tp", "fs"),
        P(),
        P("fs", "tp"),
        P("fs", "tp"),
        P("tp", "fs"),
    )
    return jax.shard_map(
        shards, mesh=mesh, in_specs=placed, out_specs=P(("rep", "fs", "tp"), None), check_vma=False
    )
```
